32 devices in a mesh: sp: 16 (over z, y, x), tp: 2 (over core).
Axes of the slice: x: 2, y: 2, z: 4, core: 2. Of those that a mesh axis runs over, the one named last changes fastest.
Arguments:
- residual: bfloat16 [4096, 2048], P(('sp', 'tp')), may hold values from -6 to 6
- query_rows: bfloat16 [4096, 1024], P('sp', 'tp'), may hold values from -141 to 141
- key_rows: bfloat16 [4096, 1024], P('sp', 'tp'), may hold values from -7.8 to 7.8
- value_rows: bfloat16 [4096, 1024], P('sp', 'tp'), may hold values from -6 to 6
- mix_lambda: float32 [8], P('tp'), may hold values from 0.3 to 0.8
- documents: int32 [4096], P('sp'), may hold values from 0 to 7, never falling along the last dimension, each value on 1 to 768 neighbouring positions
- out_weight: bfloat16 [1024, 2048], replicated, may hold values from -0.1875 to 0.1875
- norm_gain: float32 [2048], replicated, may hold values from 0.1 to 1.9
- gate_weight: bfloat16 [16, 2048, 2048], P('sp', None, 'tp'), may hold values from -0.125 to 0.125
- up_weight: bfloat16 [16, 2048, 2048], P('sp', None, 'tp'), may hold values from -0.125 to 0.125
- down_weight: bfloat16 [16, 2048, 2048], P('sp', 'tp'), may hold values from -0.125 to 0.125
- routes: int32 [4096, 2], P(('sp', 'tp')), may hold values from 0 to 15, all different within a row; in each aligned block of 128 rows (0 to 127, 128 to 255, ...) at most 32 rows name the same one
- route_weights: float32 [4096, 2], P(('sp', 'tp')), may hold values from 0.25 to 1
Outputs:
- layer_out: bfloat16 [4096, 2048], P(('sp', 'tp'))
The draws below stay inside these ranges and needn't reach their ends.
Inputs may be any that keep to these rules, and one draw needn't show every extreme that they name: `documents`: document numbers never fall along the sequence; a document covers at most 768 positions, and one covers exactly that many. `routes`: each row names two different experts. Among the rows of one index of sp+tp, no expert is named by more than 32 rows, and in every draw some expert is named by exactly 32 rows of some such block.
All inputs are finite; a program needn't handle non-finite values.
Results may differ from the reference program's by a relative error of at most 0.013.
Values may be sent and summed in bfloat16 or wider, within the bound.
A program may use at most 128 MiB of HBM per device.

```python
import math
import jax
import jax.numpy as jnp
import numpy as np
from jax import lax

D = 2048
HEADS = 8
HD = 64
VD = 128
FFE = 2048
TOK_DEV = 256
REACH = 3
TOKENS = 4096
EXPERTS = 16
CAP = 32
DOCS = 8
N_SP = 16
N_TP = 2


def drawn_pair(key):
    shape_rows = (TOKENS, HEADS * 2 * HD)
    base_query = jnp.clip(1.3 * jax.random.normal(jax.random.fold_in(key, 101), shape_rows, jnp.float32), -7.8, 7.8)
    base_keys = jnp.clip(1.3 * jax.random.normal(jax.random.fold_in(key, 102), shape_rows, jnp.float32), -7.8, 7.8)
    return (base_query, base_keys)


def draw_query_rows(key, part):
    return drawn_pair(key)[0].astype(jnp.bfloat16)


def draw_key_rows(key, part):
    return drawn_pair(key)[1].astype(jnp.bfloat16)


def steps_of(rng, dims, pieces, low, high):
    factor_of, own = 1.0, jax.random.fold_in(rng, 6)
    for axis_at, parts in pieces:
        steps = jnp.exp(jax.random.uniform(jax.random.fold_in(own, axis_at), (parts,), jnp.float32, low / len(pieces), high / len(pieces)))
        factor_of = factor_of * jnp.repeat(steps, dims[axis_at] // parts).reshape([-1 if axis == axis_at else 1 for axis in range(len(dims))])
    return factor_of


def split_up(count, total, most, slope):
    loads = [(1 << 20) // math.isqrt(rank ** slope) + 1 for rank in range(2, count + 1)]
    rest, counts = total - most - (count - 1), [1] * (count - 1)
    while rest > 0:
        candidates = [i for i in range(count - 1) if counts[i] < most]
        pool, remaining = sum([loads[i] for i in candidates]), rest
        for i in candidates:
            addition = min(most - counts[i], max(1, remaining * loads[i] // pool), rest)
            counts[i] = counts[i] + addition
            rest = rest - addition
    return np.array([most] + counts)


def uneven_parts(rng, amount, total, limit, lean):
    if amount == 2:
        one = jax.random.randint(rng, (), max(1, total - limit), min(limit, total - 1) + 1)
        return jnp.stack([one, total - one])
    lengths = jnp.asarray(split_up(amount, total, limit, lean), jnp.int32)
    pairs = (amount - 1) // 2
    donor, receiver = lengths[1:1 + 2 * pairs:2], lengths[2:2 + 2 * pairs:2]
    slack = jnp.minimum(donor - 1, limit - receiver)
    shifted = jax.random.randint(jax.random.fold_in(rng, 1), (pairs,), 0, 1 << 20) % (slack + 1)
    lengths = lengths.at[1:1 + 2 * pairs:2].set(donor - shifted).at[2:2 + 2 * pairs:2].set(receiver + shifted)
    return lengths[jax.random.permutation(jax.random.fold_in(rng, 2), amount)]


def assign_block(own_key, own, number, rows, count, top, reach, lean):
    ranking = jax.random.permutation(own_key, count)
    crowded, usual = portions_of(count, rows * top, reach, lean, True), portions_of(count, rows * top, reach, lean, False)
    places = jnp.arange(count)

    def named(sizes, offset_by):
        used = int((sizes > 0).sum())
        fixed = max(1, used // 4)
        passed = fixed + (places - fixed + offset_by * (used - fixed)) % max(1, count - fixed)
        return jnp.zeros((count,), jnp.int32).at[ranking[jnp.where(places < fixed, places, passed)]].set(jnp.asarray(sizes, jnp.int32))

    sizes = jnp.where(number % 4 == 0, named(crowded, number // 4), named(usual, number - number // 4 - 1))
    mixed = jax.random.permutation(jax.random.fold_in(own, 3), count)
    donor, sink = mixed[0:count // 2 * 2:2], mixed[1:count // 2 * 2:2]
    slack = jnp.minimum(sizes[donor] - 1, reach - sizes[sink]) // 2
    slack = jnp.where((donor == ranking[0]) | (sink == ranking[0]) | (sizes[sink] == 0), 0, jnp.maximum(slack, 0))
    passed = jax.random.randint(jax.random.fold_in(own, 4), (count // 2,), 0, 1 << 20) % (slack + 1)
    sizes = sizes.at[donor].add(-passed).at[sink].add(passed)
    items = jnp.searchsorted(jnp.cumsum(sizes), jnp.arange(rows * top), side="right").astype(jnp.int32)
    table = items.reshape(top, rows).T
    table = table[jax.random.permutation(jax.random.fold_in(own, 1), rows)]
    offset_by = jax.random.randint(jax.random.fold_in(own, 2), (rows, 1), 0, top)
    return jnp.take_along_axis(table, (jnp.arange(top)[None, :] + offset_by) % top, axis=1)


def portions_of(amount, total, reach, slope, full):
    weights = [(1 << 20) // math.isqrt(grade ** slope) + 1 for grade in range(1, amount + 1)]
    largest = reach if full else min(reach, max(-(-total // amount), total * weights[0] // sum(weights)))
    least = 1 if total - largest >= amount - 1 else 0
    holding, rest = [largest] + [least] * (amount - 1), total - largest - least * (amount - 1)
    while rest > 0:
        candidates = [i for i in range(1, amount) if holding[i] < largest] or [i for i in range(1, amount) if holding[i] < reach]
        pool, budget = sum([weights[i] for i in candidates]), rest
        for i in candidates:
            more = min(reach - holding[i], max(1, budget * weights[i] // pool), rest)
            holding[i] = holding[i] + more
            rest = rest - more
    return np.array(holding)


def normal_values(own_key, shape, deviation, limit, cuts=(), held_as=jnp.bfloat16):
    level = steps_of(own_key, shape, cuts, -0.22, 0.18) if cuts else 1.0
    values = jax.random.normal(own_key, shape, jnp.float32) * deviation * level
    return jnp.minimum(jnp.maximum(values, -limit), limit).astype(held_as)


def setup_inputs(seed: int = 0) -> dict:
    keys = jax.random.split(jax.random.key(seed), 14)
    residual = normal_values(keys[0], (TOKENS, D), 1.0, 6.0, ((0, 32),))
    query_rows = draw_query_rows(jax.random.fold_in(keys[13], 71), 0)
    key_rows = draw_key_rows(jax.random.fold_in(keys[13], 71), 0)
    value_rows = normal_values(keys[3], (TOKENS, HEADS * VD), 1.0, 6.0, ((0, 16), (1, 2)))
    mix_lambda = jnp.clip(0.3 + 0.5 * jax.random.uniform(keys[4], (HEADS,), jnp.float32) ** steps_of(keys[4], (HEADS,), ((0, 2),), -0.2, 0.2), 0.3, 0.8)
    documents = jnp.searchsorted(jnp.cumsum(uneven_parts(keys[5], DOCS, TOKENS, REACH * TOK_DEV, 0)), jnp.arange(TOKENS), side="right").astype(jnp.int32)
    out_weight = normal_values(keys[6], (HEADS * VD, D), (HEADS * VD) ** -0.5, 0.1875)
    norm_gain = jnp.clip(1.0 + 0.18 * jax.random.normal(keys[7], (D,), jnp.float32), 0.1, 1.9)
    gate_weight = normal_values(keys[8], (EXPERTS, D, FFE), D ** -0.5, 0.125, ((0, 16), (2, 2)))
    up_weight = normal_values(keys[9], (EXPERTS, D, FFE), D ** -0.5, 0.125, ((0, 16), (2, 2)))
    down_weight = normal_values(keys[10], (EXPERTS, FFE, D), FFE ** -0.5, 0.125, ((0, 16), (1, 2)))
    routes_keys = jax.random.split(jax.random.fold_in(keys[11], 1), TOKENS // (TOK_DEV // 2))
    routes_turns = jax.random.permutation(jax.random.fold_in(keys[11], 3), TOKENS // (TOK_DEV // 2))
    routes = jax.vmap(lambda own, number: assign_block(jax.random.fold_in(keys[11], 2), own, number, TOK_DEV // 2, EXPERTS, 2, CAP, 2))(routes_keys, routes_turns).reshape((TOKENS, 2))
    route_weights = jnp.clip(0.25 + 0.75 * jax.random.uniform(keys[12], (TOKENS, 2), jnp.float32) ** steps_of(keys[12], (TOKENS, 2), ((0, 32),), -0.2, 0.2), 0.25, 1.0)
    return {"residual": residual, "query_rows": query_rows, "key_rows": key_rows, "value_rows": value_rows, "mix_lambda": mix_lambda, "documents": documents, "out_weight": out_weight, "norm_gain": norm_gain, "gate_weight": gate_weight, "up_weight": up_weight, "down_weight": down_weight, "routes": routes, "route_weights": route_weights}


def rms_rows(values_in):
    return values_in * lax.rsqrt(lax.optimization_barrier(jnp.mean(values_in * values_in, axis=-1, keepdims=True)) + 1e-06)

def reference(residual, query_rows, key_rows, value_rows, mix_lambda, documents, out_weight, norm_gain, gate_weight, up_weight, down_weight, routes, route_weights):
    score_scale = HD ** (-0.5)
    queries = query_rows.reshape(TOKENS // TOK_DEV, TOK_DEV, HEADS, 2, HD)
    all_keys = key_rows.reshape(TOKENS, HEADS, 2, HD).astype(jnp.float32)
    all_values = value_rows.reshape(TOKENS, HEADS, VD).astype(jnp.float32)
    block_ids = documents.reshape(TOKENS // TOK_DEV, TOK_DEV)

    def attend(operands):
        block_query, query_ids = operands
        scores = jnp.einsum('qhcd,khcd->hcqk', block_query.astype(jnp.float32), all_keys) * score_scale
        same_document = query_ids[:, None] == documents[None, :]
        masked = jnp.where(same_document[None, None], scores, -1e+30)
        largest = lax.optimization_barrier(jnp.max(masked, axis=-1, keepdims=True))
        lifted = jnp.exp(masked - largest)
        probabilities = lifted / lax.optimization_barrier(jnp.sum(lifted, axis=-1, keepdims=True))
        weights = (probabilities[:, 0] - mix_lambda[:, None, None] * probabilities[:, 1]).astype(jnp.bfloat16)
        head_out = jnp.einsum('hqk,khd->qhd', weights.astype(jnp.float32), all_values)
        head_normed = rms_rows(head_out).astype(jnp.bfloat16)
        return head_normed.reshape(TOK_DEV, HEADS * VD)
    head_rows = lax.map(attend, (queries, block_ids)).reshape(TOKENS, HEADS * VD)
    projected = jnp.dot(head_rows, out_weight, preferred_element_type=jnp.float32)
    mixed = (residual.astype(jnp.float32) + projected).astype(jnp.bfloat16)
    normed = (rms_rows(mixed.astype(jnp.float32)) * norm_gain).astype(jnp.bfloat16)
    top_count = routes.shape[1]
    assign_count = TOKENS * top_count
    flat_routes = routes.reshape(-1)
    padded_rows = jnp.concatenate([normed, jnp.zeros((1, D), jnp.bfloat16)], axis=0)
    most_rows = N_SP * N_TP * CAP
    half_width = FFE // N_TP

    def one_expert(collected, expert):
        chosen = jnp.nonzero(flat_routes == expert, size=most_rows, fill_value=assign_count)[0].astype(jnp.int32)
        picked = padded_rows[chosen // top_count]
        gate = jnp.dot(picked, gate_weight[expert], preferred_element_type=jnp.float32)
        upward = jnp.dot(picked, up_weight[expert], preferred_element_type=jnp.float32)
        hidden = (jax.nn.silu(gate) * upward).astype(jnp.bfloat16)
        hidden_halves = hidden.reshape(most_rows, N_TP, half_width).astype(jnp.float32)
        down_halves = down_weight[expert].reshape(N_TP, half_width, D).astype(jnp.float32)
        partial_value = jnp.einsum('rhp,hpd->hrd', hidden_halves, down_halves).astype(jnp.bfloat16)
        expert_out = lax.optimization_barrier(jnp.sum(partial_value.astype(jnp.float32), axis=0)).astype(jnp.bfloat16)
        return (collected.at[chosen].set(expert_out), None)
    collected, _ = lax.scan(one_expert, jnp.zeros((assign_count + 1, D), jnp.bfloat16), jnp.arange(EXPERTS, dtype=jnp.int32))
    outputs = collected[:assign_count].reshape(TOKENS, top_count, D).astype(jnp.float32)
    weighted = lax.optimization_barrier(jnp.sum(outputs * route_weights[:, :, None], axis=1))
    return (mixed.astype(jnp.float32) + weighted).astype(jnp.bfloat16)
```

```python
import functools

import jax
import jax.numpy as jnp
from jax import lax
from jax.experimental import pallas as pl
from jax.experimental.pallas import tpu as pltpu
from jax.sharding import PartitionSpec as P

HD = 64
REACH = 3
MESH = pl.DeviceIdType.MESH
VMEM = pl.BlockSpec(memory_space=pltpu.VMEM)


def offsets_of(reach):
    return [sign * step for step in range(1, reach + 1) for sign in (1, -1)]


def halo_kernel(count, k_ref, v_ref, id_ref, k_out, v_out, id_out, send_sem, recv_sem):
    me, core = lax.axis_index("sp"), lax.axis_index("tp")
    offsets = offsets_of(REACH)
    barrier = pltpu.get_barrier_semaphore()

    def inside(offset):
        return jnp.logical_and(me + offset >= 0, me + offset < count)

    for offset in offsets:

        @pl.when(inside(offset))
        def _():
            pl.semaphore_signal(barrier, inc=1, device_id=(me + offset, core), device_id_type=MESH)

    pl.semaphore_wait(barrier, jnp.minimum(me, REACH) + jnp.minimum(count - 1 - me, REACH))

    def copies(at, offset):
        slot = REACH - offset
        return [
            pltpu.make_async_remote_copy(
                src_ref=source,
                dst_ref=target.at[slot],
                send_sem=send_sem.at[at, which],
                recv_sem=recv_sem.at[at, which],
                device_id=(me + offset, core),
                device_id_type=MESH,
            )
            for which, (source, target) in enumerate(
                ((id_ref, id_out), (k_ref, k_out), (v_ref, v_out))
            )
        ]

    for at, offset in enumerate(offsets):

        @pl.when(inside(offset))
        def _():
            for copy in copies(at, offset):
                copy.start()

    k_out[REACH] = k_ref[...]
    v_out[REACH] = v_ref[...]
    id_out[REACH] = id_ref[...]
    for offset in offsets:

        @pl.when(jnp.logical_not(inside(-offset)))
        def _():
            slot = REACH - offset
            k_out[slot] = jnp.zeros_like(k_ref)
            v_out[slot] = jnp.zeros_like(v_ref)
            id_out[slot] = jnp.full_like(id_ref, -1)

    for at, offset in enumerate(offsets):

        @pl.when(inside(-offset))
        def _():
            for copy in copies(at, offset):
                copy.wait_recv()

    for at, offset in enumerate(offsets):

        @pl.when(inside(offset))
        def _():
            for copy in copies(at, offset):
                copy.wait_send()


def halo(count, key_rows, value_rows, ids):
    slots = 2 * REACH + 1
    outs = [
        jax.ShapeDtypeStruct((slots,) + part.shape, part.dtype)
        for part in (key_rows, value_rows, ids)
    ]
    return pl.pallas_call(
        functools.partial(halo_kernel, count),
        out_shape=outs,
        in_specs=[VMEM] * 3,
        out_specs=[VMEM] * 3,
        scratch_shapes=[
            pltpu.SemaphoreType.DMA((2 * REACH, 3)),
            pltpu.SemaphoreType.DMA((2 * REACH, 3)),
        ],
        compiler_params=pltpu.CompilerParams(collective_id=0, has_side_effects=True),
        name="halo",
    )(key_rows, value_rows, ids)


def attention_kernel(lambda_ref, q_ref, k_ref, v_ref, own_ref, all_ref, out_ref):
    head = pl.program_id(0)
    query = q_ref[...]
    lane = lax.broadcasted_iota(jnp.int32, query.shape, 1)
    same = own_ref[...] == all_ref[...]
    scale = jnp.asarray(HD ** (-0.5), query.dtype)
    contract = (((1,), (1,)), ((), ()))

    def lifted(keep):
        part = jnp.where(keep, query * scale, jnp.zeros_like(query))
        scores = lax.dot_general(part, k_ref[...], contract, preferred_element_type=jnp.float32)
        masked = jnp.where(same, scores, -1e30)
        powers = jnp.exp(masked - jnp.max(masked, axis=-1, keepdims=True))
        return powers, jnp.sum(powers, axis=-1, keepdims=True)

    first, first_sum = lifted(lane < HD)
    second, second_sum = lifted(lane >= HD)
    weights = first * (1.0 / first_sum) - second * (lambda_ref[head] / second_sum)
    head_out = jnp.dot(
        weights.astype(jnp.bfloat16), v_ref[...], preferred_element_type=jnp.float32
    )
    scaled = head_out * lax.rsqrt(jnp.mean(head_out * head_out, axis=-1, keepdims=True) + 1e-06)
    out_ref[...] = scaled.astype(jnp.bfloat16)


def attention(query_rows, all_keys, all_values, own_ids, all_ids, mix_lambda):
    length, width = query_rows.shape
    heads = mix_lambda.shape[0]
    wide, keys = width // heads, all_keys.shape[0]
    value_dim = all_values.shape[1] // heads
    rows = min(length, 128)
    return pl.pallas_call(
        attention_kernel,
        grid=(heads, length // rows),
        out_shape=jax.ShapeDtypeStruct((length, heads * value_dim), jnp.bfloat16),
        in_specs=[
            pl.BlockSpec(memory_space=pltpu.SMEM),
            pl.BlockSpec((rows, wide), lambda h, r: (r, h)),
            pl.BlockSpec((keys, wide), lambda h, r: (0, h)),
            pl.BlockSpec((keys, value_dim), lambda h, r: (0, h)),
            pl.BlockSpec((rows, 1), lambda h, r: (r, 0)),
            pl.BlockSpec((1, keys), lambda h, r: (0, 0)),
        ],
        out_specs=pl.BlockSpec((rows, value_dim), lambda h, r: (r, h)),
        name="attention",
    )(mix_lambda, query_rows, all_keys, all_values, own_ids, all_ids)


def greet_all(count, me, core):
    barrier = pltpu.get_barrier_semaphore()
    pl.semaphore_signal(barrier, inc=1, device_id=(me, 1 - core), device_id_type=MESH)

    @pl.loop(1, count)
    def _(step):
        pl.semaphore_signal(
            barrier, inc=1, device_id=((me + step) % count, core), device_id_type=MESH
        )

    pl.semaphore_wait(barrier, count)


def dispatch_kernel(count, out_ref, rows_ref, send_sem, recv_sem, pass_sem, come_sem, own_sem):
    me, core = lax.axis_index("sp"), lax.axis_index("tp")
    greet_all(count, me, core)

    def across(step):
        target = (me + step) % count
        return pltpu.make_async_remote_copy(
            src_ref=out_ref.at[target],
            dst_ref=rows_ref.at[core, me],
            send_sem=send_sem.at[step],
            recv_sem=recv_sem.at[step],
            device_id=(target, core),
            device_id_type=MESH,
        )

    def arrived(step):
        source = (me - step + count) % count
        return pltpu.make_async_remote_copy(
            src_ref=rows_ref.at[core, source],
            dst_ref=rows_ref.at[core, source],
            send_sem=pass_sem.at[step],
            recv_sem=recv_sem.at[step],
            device_id=(me, 1 - core),
            device_id_type=MESH,
        )

    def beside(step, side, source_ref=None):
        source = (me - step + count) % count
        return pltpu.make_async_remote_copy(
            src_ref=rows_ref.at[side, source] if source_ref is None else source_ref,
            dst_ref=rows_ref.at[side, source],
            send_sem=pass_sem.at[step],
            recv_sem=come_sem.at[step],
            device_id=(me, 1 - core),
            device_id_type=MESH,
        )

    @pl.loop(1, count)
    def _(step):
        across(step).start()

    own = pltpu.make_async_copy(out_ref.at[me], rows_ref.at[core, me], own_sem)
    own.start()
    beside(0, core, out_ref.at[me]).start()

    @pl.loop(1, count)
    def _(step):
        arrived(step).wait_recv()
        beside(step, core).start()

    own.wait()

    @pl.loop(0, count)
    def _(step):
        beside(step, 1 - core).wait_recv()
        beside(step, core).wait_send()

    @pl.loop(1, count)
    def _(step):
        across(step).wait_send()


def dispatch(count, outgoing):
    return pl.pallas_call(
        functools.partial(dispatch_kernel, count),
        out_shape=jax.ShapeDtypeStruct((2,) + outgoing.shape, outgoing.dtype),
        in_specs=[VMEM],
        out_specs=VMEM,
        scratch_shapes=[pltpu.SemaphoreType.DMA((count,))] * 4 + [pltpu.SemaphoreType.DMA],
        compiler_params=pltpu.CompilerParams(collective_id=1, has_side_effects=True),
        name="dispatch",
    )(outgoing)


def give_back_kernel(
    count, part_ref, back_ref, far_ref, sum_ref, pass_sem, come_sem, send_sem, recv_sem
):
    me, core = lax.axis_index("sp"), lax.axis_index("tp")
    greet_all(count, me, core)

    def beside(step):
        at = (me + step) % count
        return pltpu.make_async_remote_copy(
            src_ref=part_ref.at[1 - core, at],
            dst_ref=far_ref.at[at],
            send_sem=pass_sem.at[step],
            recv_sem=come_sem.at[step],
            device_id=(me, 1 - core),
            device_id_type=MESH,
        )

    def across(step):
        target = (me + step) % count
        return pltpu.make_async_remote_copy(
            src_ref=sum_ref.at[target],
            dst_ref=back_ref.at[me],
            send_sem=send_sem.at[step],
            recv_sem=recv_sem.at[step],
            device_id=(target, core),
            device_id_type=MESH,
        )

    def arrived(step):
        source = (me - step + count) % count
        return pltpu.make_async_remote_copy(
            src_ref=sum_ref.at[source],
            dst_ref=back_ref.at[source],
            send_sem=send_sem.at[step],
            recv_sem=recv_sem.at[step],
            device_id=(source, core),
            device_id_type=MESH,
        )

    def total(step):
        at = (me + step) % count
        beside(step).wait_recv()
        own = part_ref[core, at].astype(jnp.float32)
        return (own + far_ref[at].astype(jnp.float32)).astype(sum_ref.dtype), at

    @pl.loop(1, count)
    def _(step):
        beside(step).start()

    beside(0).start()

    @pl.loop(1, count)
    def _(step):
        value, at = total(step)
        sum_ref[at] = value

        @pl.when(step > 1)
        def _():
            across(step - 1).start()

    value, at = total(0)
    back_ref[at] = value
    across(count - 1).start()

    @pl.loop(1, count)
    def _(step):
        arrived(step).wait_recv()
        across(step).wait_send()

    @pl.loop(0, count)
    def _(step):
        beside(step).wait_send()


def give_back(count, partial):
    shape = partial.shape[1:]
    return pl.pallas_call(
        functools.partial(give_back_kernel, count),
        out_shape=jax.ShapeDtypeStruct(shape, partial.dtype),
        in_specs=[VMEM],
        out_specs=VMEM,
        scratch_shapes=[pltpu.VMEM(shape, partial.dtype)] * 2
        + [pltpu.SemaphoreType.DMA((count,))] * 4,
        compiler_params=pltpu.CompilerParams(collective_id=2, has_side_effects=True),
        name="give_back",
    )(partial)


def slots_of(routes, experts, capacity):
    flat_routes = routes.reshape(-1)
    table = (flat_routes[:, None] == jnp.arange(experts, dtype=jnp.int32)[None, :]).astype(
        jnp.float32
    )
    count = table.shape[0]
    before = jnp.tril(jnp.ones((count, count), jnp.bfloat16), -1)
    earlier = jnp.dot(before, table.astype(jnp.bfloat16), preferred_element_type=jnp.float32)
    rank = jnp.sum(earlier * table, axis=1).astype(jnp.int32)
    return (flat_routes * capacity + rank).reshape(routes.shape)


def on_device(
    residual,
    query_rows,
    key_rows,
    value_rows,
    mix_lambda,
    documents,
    out_weight,
    norm_gain,
    gate_weight,
    up_weight,
    down_weight,
    routes,
    route_weights,
):
    length = query_rows.shape[0]
    model_width = residual.shape[1]
    experts = lax.axis_size("sp")
    capacity = 2 * length // experts
    top_count = routes.shape[1]
    keys, values, ids = halo(experts, key_rows, value_rows, documents.reshape(1, length))
    merged = attention(
        query_rows,
        keys.reshape(-1, keys.shape[-1]),
        values.reshape(-1, values.shape[-1]),
        documents.reshape(length, 1),
        ids.reshape(1, -1),
        mix_lambda,
    )
    token_heads = lax.all_to_all(merged, "tp", split_axis=0, concat_axis=1, tiled=True)
    projected = jnp.dot(token_heads, out_weight, preferred_element_type=jnp.float32)
    mixed = (residual.astype(jnp.float32) + projected).astype(jnp.bfloat16)
    mixed_wide = mixed.astype(jnp.float32)
    normed = (
        mixed_wide
        * lax.rsqrt(jnp.mean(mixed_wide * mixed_wide, axis=-1, keepdims=True) + 1e-06)
        * norm_gain
    ).astype(jnp.bfloat16)
    slots = slots_of(routes, experts, capacity)
    places = jnp.arange(experts * capacity, dtype=jnp.int32)
    spread = jnp.any(slots[None, :, :] == places[:, None, None], axis=-1).astype(jnp.bfloat16)
    outgoing = jnp.dot(spread, normed, preferred_element_type=jnp.float32).astype(jnp.bfloat16)
    rows_all = dispatch(experts, outgoing.reshape(experts, capacity, model_width))
    shape = rows_all.shape
    rows_all = rows_all.reshape(-1, model_width)
    gate = jnp.dot(rows_all, gate_weight[0], preferred_element_type=jnp.float32)
    upward = jnp.dot(rows_all, up_weight[0], preferred_element_type=jnp.float32)
    hidden = (jax.nn.silu(gate) * upward).astype(jnp.bfloat16)
    partial = jnp.dot(hidden, down_weight[0], preferred_element_type=jnp.float32).astype(
        jnp.bfloat16
    )
    returned = give_back(experts, partial.reshape(shape)).reshape(-1, model_width)
    weighted = 0.0
    for which in range(top_count):
        pick = (slots[:, which][:, None] == places[None, :]).astype(jnp.bfloat16)
        picked = jnp.dot(pick, returned, preferred_element_type=jnp.float32)
        weighted = weighted + picked * route_weights[:, which][:, None]
    return (mixed_wide + weighted).astype(jnp.bfloat16)


def solution(mesh):
    placed = (
        P(("sp", "tp"), None),
        P("sp", "tp"),
        P("sp", "tp"),
        P("sp", "tp"),
        P("tp"),
        P("sp"),
        P(),
        P(),
        P("sp", None, "tp"),
        P("sp", None, "tp"),
        P("sp", "tp", None),
        P(("sp", "tp"), None),
        P(("sp", "tp"), None),
    )
    return jax.shard_map(
        on_device, mesh=mesh, in_specs=placed, out_specs=P(("sp", "tp"), None), check_vma=False
    )
```

```python
import functools

import jax
import jax.numpy as jnp
from jax import lax
from jax.experimental import pallas as pl
from jax.experimental.pallas import tpu as pltpu
from jax.sharding import PartitionSpec as P

HD = 64
REACH = 3
MESH = pl.DeviceIdType.MESH
VMEM = pl.BlockSpec(memory_space=pltpu.VMEM)


def offsets_of(reach):
    return [sign * step for step in range(1, reach + 1) for sign in (1, -1)]


def halo_kernel(
    count, k_ref, v_ref, id_ref, k_out, v_out, id_out, send_sem, recv_sem, pass_sem
):
    me, core = lax.axis_index("sp"), lax.axis_index("tp")
    offsets = offsets_of(REACH)
    group = REACH + 1
    barrier = pltpu.get_barrier_semaphore()

    def inside(offset):
        return jnp.logical_and(me + offset >= 0, me + offset < count)

    for offset in offsets_of(group):

        @pl.when(inside(offset))
        def _():
            pl.semaphore_signal(barrier, inc=1, device_id=(me + offset, core), device_id_type=MESH)

    pl.semaphore_wait(barrier, jnp.minimum(me, group) + jnp.minimum(count - 1 - me, group))

    place = me % group

    def near(offset):
        return jnp.logical_and(place + offset >= 0, place + offset < group)

    def opposite(offset):
        return place + (place + offset + group) % group == group - 1

    def copies(at, offset):
        slot = REACH - offset
        return [
            pltpu.make_async_remote_copy(
                src_ref=source,
                dst_ref=target.at[slot],
                send_sem=send_sem.at[at, which],
                recv_sem=recv_sem.at[at, which],
                device_id=(me + offset, core),
                device_id_type=MESH,
            )
            for which, (source, target) in enumerate(
                ((id_ref, id_out), (k_ref, k_out), (v_ref, v_out))
            )
        ]

    def passes(at, offset):
        hop = group if offset < 0 else -group
        beyond = offset + hop
        return [
            pltpu.make_async_remote_copy(
                src_ref=part.at[REACH - offset],
                dst_ref=part.at[REACH - beyond],
                send_sem=pass_sem.at[at, which],
                recv_sem=recv_sem.at[offsets.index(beyond), which],
                device_id=(me + hop, core),
                device_id_type=MESH,
            )
            for which, part in enumerate((id_out, k_out, v_out))
        ]

    def sends(offset):
        return jnp.logical_and(inside(offset), jnp.logical_or(near(offset), opposite(offset)))

    def relays(offset):
        hop = group if offset < 0 else -group
        aligned = jnp.logical_and(inside(-offset), near(-offset))
        aligned = jnp.logical_and(aligned, jnp.logical_not(opposite(-offset)))
        return jnp.logical_and(aligned, inside(hop))

    for at, offset in enumerate(offsets):

        @pl.when(sends(offset))
        def _():
            for copy in copies(at, offset):
                copy.start()

    k_out[REACH] = k_ref[...]
    v_out[REACH] = v_ref[...]
    id_out[REACH] = id_ref[...]
    for offset in offsets:

        @pl.when(jnp.logical_not(inside(-offset)))
        def _():
            slot = REACH - offset
            k_out[slot] = jnp.zeros_like(k_ref)
            v_out[slot] = jnp.zeros_like(v_ref)
            id_out[slot] = jnp.full_like(id_ref, -1)

    for which in range(3):
        for at, offset in enumerate(offsets):

            @pl.when(relays(offset))
            def _():
                copies(at, offset)[which].wait_recv()
                passes(at, offset)[which].start()

    for at, offset in enumerate(offsets):

        @pl.when(jnp.logical_and(inside(-offset), jnp.logical_not(relays(offset))))
        def _():
            for copy in copies(at, offset):
                copy.wait_recv()

    for at, offset in enumerate(offsets):

        @pl.when(sends(offset))
        def _():
            for copy in copies(at, offset):
                copy.wait_send()

        @pl.when(relays(offset))
        def _():
            for copy in passes(at, offset):
                copy.wait_send()


def halo(count, key_rows, value_rows, ids):
    slots = 2 * REACH + 1
    outs = [
        jax.ShapeDtypeStruct((slots,) + part.shape, part.dtype)
        for part in (key_rows, value_rows, ids)
    ]
    return pl.pallas_call(
        functools.partial(halo_kernel, count),
        out_shape=outs,
        in_specs=[VMEM] * 3,
        out_specs=[VMEM] * 3,
        scratch_shapes=[pltpu.SemaphoreType.DMA((2 * REACH, 3))] * 3,
        compiler_params=pltpu.CompilerParams(collective_id=0, has_side_effects=True),
        name="halo",
    )(key_rows, value_rows, ids)


def attention_kernel(lambda_ref, q_ref, k_ref, v_ref, own_ref, all_ref, out_ref):
    head = pl.program_id(0)
    query = q_ref[...]
    lane = lax.broadcasted_iota(jnp.int32, query.shape, 1)
    same = own_ref[...] == all_ref[...]
    scale = jnp.asarray(HD ** (-0.5), query.dtype)
    contract = (((1,), (1,)), ((), ()))

    def lifted(keep):
        part = jnp.where(keep, query * scale, jnp.zeros_like(query))
        scores = lax.dot_general(part, k_ref[...], contract, preferred_element_type=jnp.float32)
        masked = jnp.where(same, scores, -1e30)
        powers = jnp.exp(masked - jnp.max(masked, axis=-1, keepdims=True))
        return powers, jnp.sum(powers, axis=-1, keepdims=True)

    first, first_sum = lifted(lane < HD)
    second, second_sum = lifted(lane >= HD)
    weights = first * (1.0 / first_sum) - second * (lambda_ref[head] / second_sum)
    head_out = jnp.dot(
        weights.astype(jnp.bfloat16), v_ref[...], preferred_element_type=jnp.float32
    )
    scaled = head_out * lax.rsqrt(jnp.mean(head_out * head_out, axis=-1, keepdims=True) + 1e-06)
    out_ref[...] = scaled.astype(jnp.bfloat16)


def attention(query_rows, all_keys, all_values, own_ids, all_ids, mix_lambda):
    length, width = query_rows.shape
    heads = mix_lambda.shape[0]
    wide, keys = width // heads, all_keys.shape[0]
    value_dim = all_values.shape[1] // heads
    rows = min(length, 128)
    return pl.pallas_call(
        attention_kernel,
        grid=(heads, length // rows),
        out_shape=jax.ShapeDtypeStruct((length, heads * value_dim), jnp.bfloat16),
        in_specs=[
            pl.BlockSpec(memory_space=pltpu.SMEM),
            pl.BlockSpec((rows, wide), lambda h, r: (r, h)),
            pl.BlockSpec((keys, wide), lambda h, r: (0, h)),
            pl.BlockSpec((keys, value_dim), lambda h, r: (0, h)),
            pl.BlockSpec((rows, 1), lambda h, r: (r, 0)),
            pl.BlockSpec((1, keys), lambda h, r: (0, 0)),
        ],
        out_specs=pl.BlockSpec((rows, value_dim), lambda h, r: (r, h)),
        name="attention",
    )(mix_lambda, query_rows, all_keys, all_values, own_ids, all_ids)


def greet_all(count, me, core):
    barrier = pltpu.get_barrier_semaphore()
    pl.semaphore_signal(barrier, inc=1, device_id=(me, 1 - core), device_id_type=MESH)

    @pl.loop(1, count)
    def _(step):
        pl.semaphore_signal(
            barrier, inc=1, device_id=((me + step) % count, core), device_id_type=MESH
        )

    pl.semaphore_wait(barrier, count)


def dispatch_kernel(count, out_ref, rows_ref, send_sem, recv_sem, pass_sem, come_sem, own_sem):
    me, core = lax.axis_index("sp"), lax.axis_index("tp")
    greet_all(count, me, core)

    def across(step):
        target = (me + step) % count
        return pltpu.make_async_remote_copy(
            src_ref=out_ref.at[target],
            dst_ref=rows_ref.at[core, me],
            send_sem=send_sem.at[step],
            recv_sem=recv_sem.at[step],
            device_id=(target, core),
            device_id_type=MESH,
        )

    def arrived(step):
        source = (me - step + count) % count
        return pltpu.make_async_remote_copy(
            src_ref=rows_ref.at[core, source],
            dst_ref=rows_ref.at[core, source],
            send_sem=pass_sem.at[step],
            recv_sem=recv_sem.at[step],
            device_id=(me, 1 - core),
            device_id_type=MESH,
        )

    def beside(step, side, source_ref=None):
        source = (me - step + count) % count
        return pltpu.make_async_remote_copy(
            src_ref=rows_ref.at[side, source] if source_ref is None else source_ref,
            dst_ref=rows_ref.at[side, source],
            send_sem=pass_sem.at[step],
            recv_sem=come_sem.at[step],
            device_id=(me, 1 - core),
            device_id_type=MESH,
        )

    @pl.loop(1, count)
    def _(step):
        across(step).start()

    own = pltpu.make_async_copy(out_ref.at[me], rows_ref.at[core, me], own_sem)
    own.start()
    beside(0, core, out_ref.at[me]).start()

    @pl.loop(1, count)
    def _(step):
        arrived(step).wait_recv()
        beside(step, core).start()

    own.wait()

    @pl.loop(0, count)
    def _(step):
        beside(step, 1 - core).wait_recv()
        beside(step, core).wait_send()

    @pl.loop(1, count)
    def _(step):
        across(step).wait_send()


def dispatch(count, outgoing):
    return pl.pallas_call(
        functools.partial(dispatch_kernel, count),
        out_shape=jax.ShapeDtypeStruct((2,) + outgoing.shape, outgoing.dtype),
        in_specs=[VMEM],
        out_specs=VMEM,
        scratch_shapes=[pltpu.SemaphoreType.DMA((count,))] * 4 + [pltpu.SemaphoreType.DMA],
        compiler_params=pltpu.CompilerParams(collective_id=1, has_side_effects=True),
        name="dispatch",
    )(outgoing)


def give_back_kernel(
    count, part_ref, back_ref, far_ref, sum_ref, pass_sem, come_sem, send_sem, recv_sem
):
    me, core = lax.axis_index("sp"), lax.axis_index("tp")
    greet_all(count, me, core)

    def beside(step):
        at = (me + step) % count
        return pltpu.make_async_remote_copy(
            src_ref=part_ref.at[1 - core, at],
            dst_ref=far_ref.at[at],
            send_sem=pass_sem.at[step],
            recv_sem=come_sem.at[step],
            device_id=(me, 1 - core),
            device_id_type=MESH,
        )

    def across(step):
        target = (me + step) % count
        return pltpu.make_async_remote_copy(
            src_ref=sum_ref.at[target],
            dst_ref=back_ref.at[me],
            send_sem=send_sem.at[step],
            recv_sem=recv_sem.at[step],
            device_id=(target, core),
            device_id_type=MESH,
        )

    def arrived(step):
        source = (me - step + count) % count
        return pltpu.make_async_remote_copy(
            src_ref=sum_ref.at[source],
            dst_ref=back_ref.at[source],
            send_sem=send_sem.at[step],
            recv_sem=recv_sem.at[step],
            device_id=(source, core),
            device_id_type=MESH,
        )

    def total(step):
        at = (me + step) % count
        beside(step).wait_recv()
        own = part_ref[core, at].astype(jnp.float32)
        return (own + far_ref[at].astype(jnp.float32)).astype(sum_ref.dtype), at

    def far_first(turn):
        return (turn + count // 2 - 2) % (count - 1) + 1

    @pl.loop(1, count)
    def _(turn):
        beside(far_first(turn)).start()

    beside(0).start()

    @pl.loop(1, count)
    def _(turn):
        value, at = total(far_first(turn))
        sum_ref[at] = value

        @pl.when(turn > 1)
        def _():
            across(far_first(turn - 1)).start()

    value, at = total(0)
    back_ref[at] = value
    across(far_first(count - 1)).start()

    @pl.loop(1, count)
    def _(step):
        arrived(step).wait_recv()
        across(step).wait_send()

    @pl.loop(0, count)
    def _(step):
        beside(step).wait_send()


def give_back(count, partial):
    shape = partial.shape[1:]
    return pl.pallas_call(
        functools.partial(give_back_kernel, count),
        out_shape=jax.ShapeDtypeStruct(shape, partial.dtype),
        in_specs=[VMEM],
        out_specs=VMEM,
        scratch_shapes=[pltpu.VMEM(shape, partial.dtype)] * 2
        + [pltpu.SemaphoreType.DMA((count,))] * 4,
        compiler_params=pltpu.CompilerParams(collective_id=2, has_side_effects=True),
        name="give_back",
    )(partial)


def slots_of(routes, experts, capacity):
    flat_routes = routes.reshape(-1)
    table = (flat_routes[:, None] == jnp.arange(experts, dtype=jnp.int32)[None, :]).astype(
        jnp.float32
    )
    count = table.shape[0]
    before = jnp.tril(jnp.ones((count, count), jnp.bfloat16), -1)
    earlier = jnp.dot(before, table.astype(jnp.bfloat16), preferred_element_type=jnp.float32)
    rank = jnp.sum(earlier * table, axis=1).astype(jnp.int32)
    return (flat_routes * capacity + rank).reshape(routes.shape)


def on_device(
    residual,
    query_rows,
    key_rows,
    value_rows,
    mix_lambda,
    documents,
    out_weight,
    norm_gain,
    gate_weight,
    up_weight,
    down_weight,
    routes,
    route_weights,
):
    length = query_rows.shape[0]
    model_width = residual.shape[1]
    experts = lax.axis_size("sp")
    capacity = 2 * length // experts
    top_count = routes.shape[1]
    keys, values, ids = halo(experts, key_rows, value_rows, documents.reshape(1, length))
    merged = attention(
        query_rows,
        keys.reshape(-1, keys.shape[-1]),
        values.reshape(-1, values.shape[-1]),
        documents.reshape(length, 1),
        ids.reshape(1, -1),
        mix_lambda,
    )
    token_heads = lax.all_to_all(merged, "tp", split_axis=0, concat_axis=1, tiled=True)
    projected = jnp.dot(token_heads, out_weight, preferred_element_type=jnp.float32)
    mixed = (residual.astype(jnp.float32) + projected).astype(jnp.bfloat16)
    mixed_wide = mixed.astype(jnp.float32)
    normed = (
        mixed_wide
        * lax.rsqrt(jnp.mean(mixed_wide * mixed_wide, axis=-1, keepdims=True) + 1e-06)
        * norm_gain
    ).astype(jnp.bfloat16)
    slots = slots_of(routes, experts, capacity)
    places = jnp.arange(experts * capacity, dtype=jnp.int32)
    spread = jnp.any(slots[None, :, :] == places[:, None, None], axis=-1).astype(jnp.bfloat16)
    outgoing = jnp.dot(spread, normed, preferred_element_type=jnp.float32).astype(jnp.bfloat16)
    rows_all = dispatch(experts, outgoing.reshape(experts, capacity, model_width))
    shape = rows_all.shape
    rows_all = rows_all.reshape(-1, model_width)
    gate = jnp.dot(rows_all, gate_weight[0], preferred_element_type=jnp.float32)
    upward = jnp.dot(rows_all, up_weight[0], preferred_element_type=jnp.float32)
    hidden = (jax.nn.silu(gate) * upward).astype(jnp.bfloat16)
    partial = jnp.dot(hidden, down_weight[0], preferred_element_type=jnp.float32).astype(
        jnp.bfloat16
    )
    returned = give_back(experts, partial.reshape(shape)).reshape(-1, model_width)
    weighted = 0.0
    for which in range(top_count):
        pick = (slots[:, which][:, None] == places[None, :]).astype(jnp.bfloat16)
        picked = jnp.dot(pick, returned, preferred_element_type=jnp.float32)
        weighted = weighted + picked * route_weights[:, which][:, None]
    return (mixed_wide + weighted).astype(jnp.bfloat16)


def solution(mesh):
    placed = (
        P(("sp", "tp"), None),
        P("sp", "tp"),
        P("sp", "tp"),
        P("sp", "tp"),
        P("tp"),
        P("sp"),
        P(),
        P(),
        P("sp", None, "tp"),
        P("sp", None, "tp"),
        P("sp", "tp", None),
        P(("sp", "tp"), None),
        P(("sp", "tp"), None),
    )
    return jax.shard_map(
        on_device, mesh=mesh, in_specs=placed, out_specs=P(("sp", "tp"), None), check_vma=False
    )
```

```python
import functools

import jax
import jax.numpy as jnp
from jax import lax
from jax.experimental import pallas as pl
from jax.experimental.pallas import tpu as pltpu
from jax.sharding import PartitionSpec as P

HD = 64
REACH = 3
MESH = pl.DeviceIdType.MESH
VMEM = pl.BlockSpec(memory_space=pltpu.VMEM)


def offsets_of(reach):
    return [sign * step for step in range(1, reach + 1) for sign in (1, -1)]


def halo_kernel(
    count, k_ref, v_ref, id_ref, k_out, v_out, id_out, send_sem, recv_sem, pass_sem
):
    me, core = lax.axis_index("sp"), lax.axis_index("tp")
    offsets = offsets_of(REACH)
    group = REACH + 1
    barrier = pltpu.get_barrier_semaphore()

    def inside(offset):
        return jnp.logical_and(me + offset >= 0, me + offset < count)

    for offset in offsets_of(group):

        @pl.when(inside(offset))
        def _():
            pl.semaphore_signal(barrier, inc=1, device_id=(me + offset, core), device_id_type=MESH)

    pl.semaphore_wait(barrier, jnp.minimum(me, group) + jnp.minimum(count - 1 - me, group))

    place = me % group

    def near(offset):
        return jnp.logical_and(place + offset >= 0, place + offset < group)

    def opposite(offset):
        return place + (place + offset + group) % group == group - 1

    def copies(at, offset):
        slot = REACH - offset
        return [
            pltpu.make_async_remote_copy(
                src_ref=source,
                dst_ref=target.at[slot],
                send_sem=send_sem.at[at, which],
                recv_sem=recv_sem.at[at, which],
                device_id=(me + offset, core),
                device_id_type=MESH,
            )
            for which, (source, target) in enumerate(
                ((id_ref, id_out), (k_ref, k_out), (v_ref, v_out))
            )
        ]

    def passes(at, offset):
        hop = group if offset < 0 else -group
        beyond = offset + hop
        return [
            pltpu.make_async_remote_copy(
                src_ref=part.at[REACH - offset],
                dst_ref=part.at[REACH - beyond],
                send_sem=pass_sem.at[at, which],
                recv_sem=recv_sem.at[offsets.index(beyond), which],
                device_id=(me + hop, core),
                device_id_type=MESH,
            )
            for which, part in enumerate((id_out, k_out, v_out))
        ]

    def sends(offset):
        return jnp.logical_and(inside(offset), jnp.logical_or(near(offset), opposite(offset)))

    def relays(offset):
        hop = group if offset < 0 else -group
        aligned = jnp.logical_and(inside(-offset), near(-offset))
        aligned = jnp.logical_and(aligned, jnp.logical_not(opposite(-offset)))
        return jnp.logical_and(aligned, inside(hop))

    for at, offset in enumerate(offsets):

        @pl.when(sends(offset))
        def _():
            for copy in copies(at, offset):
                copy.start()

    k_out[REACH] = k_ref[...]
    v_out[REACH] = v_ref[...]
    id_out[REACH] = id_ref[...]
    for offset in offsets:

        @pl.when(jnp.logical_not(inside(-offset)))
        def _():
            slot = REACH - offset
            k_out[slot] = jnp.zeros_like(k_ref)
            v_out[slot] = jnp.zeros_like(v_ref)
            id_out[slot] = jnp.full_like(id_ref, -1)

    for which in range(3):
        for at, offset in enumerate(offsets):

            @pl.when(relays(offset))
            def _():
                copies(at, offset)[which].wait_recv()
                passes(at, offset)[which].start()

    for at, offset in enumerate(offsets):

        @pl.when(jnp.logical_and(inside(-offset), jnp.logical_not(relays(offset))))
        def _():
            for copy in copies(at, offset):
                copy.wait_recv()

    for at, offset in enumerate(offsets):

        @pl.when(sends(offset))
        def _():
            for copy in copies(at, offset):
                copy.wait_send()

        @pl.when(relays(offset))
        def _():
            for copy in passes(at, offset):
                copy.wait_send()


def halo(count, key_rows, value_rows, ids):
    slots = 2 * REACH + 1
    outs = [
        jax.ShapeDtypeStruct((slots,) + part.shape, part.dtype)
        for part in (key_rows, value_rows, ids)
    ]
    return pl.pallas_call(
        functools.partial(halo_kernel, count),
        out_shape=outs,
        in_specs=[VMEM] * 3,
        out_specs=[VMEM] * 3,
        scratch_shapes=[pltpu.SemaphoreType.DMA((2 * REACH, 3))] * 3,
        compiler_params=pltpu.CompilerParams(collective_id=0, has_side_effects=True),
        name="halo",
    )(key_rows, value_rows, ids)


def attention_kernel(lambda_ref, q_ref, k_ref, v_ref, own_ref, all_ref, out_ref):
    head = pl.program_id(0)
    query = q_ref[...]
    lane = lax.broadcasted_iota(jnp.int32, query.shape, 1)
    same = own_ref[...] == all_ref[...]
    scale = jnp.asarray(HD ** (-0.5), query.dtype)
    contract = (((1,), (1,)), ((), ()))

    def lifted(keep):
        part = jnp.where(keep, query * scale, jnp.zeros_like(query))
        scores = lax.dot_general(part, k_ref[...], contract, preferred_element_type=jnp.float32)
        masked = jnp.where(same, scores, -1e30)
        powers = jnp.exp(masked - jnp.max(masked, axis=-1, keepdims=True))
        return powers, jnp.sum(powers, axis=-1, keepdims=True)

    first, first_sum = lifted(lane < HD)
    second, second_sum = lifted(lane >= HD)
    weights = first * (1.0 / first_sum) - second * (lambda_ref[head] / second_sum)
    head_out = jnp.dot(
        weights.astype(jnp.bfloat16), v_ref[...], preferred_element_type=jnp.float32
    )
    scaled = head_out * lax.rsqrt(jnp.mean(head_out * head_out, axis=-1, keepdims=True) + 1e-06)
    out_ref[...] = scaled.astype(jnp.bfloat16)


def attention(query_rows, all_keys, all_values, own_ids, all_ids, mix_lambda):
    length, width = query_rows.shape
    heads = mix_lambda.shape[0]
    wide, keys = width // heads, all_keys.shape[0]
    value_dim = all_values.shape[1] // heads
    rows = min(length, 128)
    return pl.pallas_call(
        attention_kernel,
        grid=(heads, length // rows),
        out_shape=jax.ShapeDtypeStruct((length, heads * value_dim), jnp.bfloat16),
        in_specs=[
            pl.BlockSpec(memory_space=pltpu.SMEM),
            pl.BlockSpec((rows, wide), lambda h, r: (r, h)),
            pl.BlockSpec((keys, wide), lambda h, r: (0, h)),
            pl.BlockSpec((keys, value_dim), lambda h, r: (0, h)),
            pl.BlockSpec((rows, 1), lambda h, r: (r, 0)),
            pl.BlockSpec((1, keys), lambda h, r: (0, 0)),
        ],
        out_specs=pl.BlockSpec((rows, value_dim), lambda h, r: (r, h)),
        name="attention",
    )(mix_lambda, query_rows, all_keys, all_values, own_ids, all_ids)


def greet_all(count, me, core):
    barrier = pltpu.get_barrier_semaphore()
    pl.semaphore_signal(barrier, inc=1, device_id=(me, 1 - core), device_id_type=MESH)

    @pl.loop(1, count)
    def _(step):
        pl.semaphore_signal(
            barrier, inc=1, device_id=((me + step) % count, core), device_id_type=MESH
        )

    pl.semaphore_wait(barrier, count)


def experts_kernel(
    count,
    out_ref,
    gate_hbm,
    up_hbm,
    down_hbm,
    back_ref,
    rows_ref,
    part_ref,
    far_ref,
    sum_ref,
    hidden_ref,
    gate_ref,
    up_ref,
    down_ref,
    load_sem,
    own_sem,
    send_sem,
    recv_sem,
    pass_sem,
    come_sem,
    swap_sem,
    half_sem,
    give_sem,
    take_sem,
):
    me, core = lax.axis_index("sp"), lax.axis_index("tp")
    per = rows_ref.shape[2]
    groups = count // per
    layer, place = me // per, me % per
    greet_all(count, me, core)

    def ahead(g, j):
        return (layer + g) % groups * per + (place + j) % per

    def behind(g, j):
        return (layer - g + groups) % groups * per + (place - j + per) % per

    def remote(source, target, sent, came, at, side):
        return pltpu.make_async_remote_copy(
            src_ref=source,
            dst_ref=target,
            send_sem=sent,
            recv_sem=came,
            device_id=(at, side),
            device_id_type=MESH,
        )

    def across(g, j):
        at = ahead(g, j)
        return remote(
            out_ref.at[at], rows_ref.at[g, core, j], send_sem.at[g, j], recv_sem.at[g, j], at, core
        )

    def forward(g, j, side):
        block = rows_ref.at[g, side, j]
        return remote(block, block, pass_sem.at[g, j], come_sem.at[g, j], me, 1 - core)

    def swap(g):
        return remote(
            part_ref.at[g, 1 - core], far_ref.at[g], swap_sem.at[g], half_sem.at[g], me, 1 - core
        )

    def home(g, j):
        at = behind(g, j)
        return remote(
            sum_ref.at[g, j], back_ref.at[me], give_sem.at[g, j], take_sem.at[g, j], at, core
        )

    def came_home(g, j):
        at = ahead(g, j)
        return remote(
            sum_ref.at[g, j], back_ref.at[at], give_sem.at[g, j], take_sem.at[g, j], at, core
        )

    own = pltpu.make_async_copy(out_ref.at[me], rows_ref.at[0, core, 0], own_sem)
    own.start()

    @pl.loop(1, count)
    def _(step):
        across(step // per, step % per).start()

    loads = [
        pltpu.make_async_copy(source, target, load_sem.at[which])
        for which, (source, target) in enumerate(
            ((gate_hbm, gate_ref), (up_hbm, up_ref), (down_hbm, down_ref))
        )
    ]
    for load in loads:
        load.start()
    own.wait()
    forward(0, 0, core).start()

    @pl.loop(0, groups)
    def _(g):
        for j in range(per):

            @pl.when(g + j > 0)
            def _():
                across(g, j).wait_recv()
                forward(g, j, core).start()

        for j in range(per):
            forward(g, j, 1 - core).wait_recv()

        @pl.when(g == 0)
        def _():
            for load in loads:
                load.wait()

        rows, width = hidden_ref.shape
        model = down_ref.shape[1]
        wide = min(256, width)

        @pl.loop(0, width // wide)
        def _(c):
            cut = pl.ds(pl.multiple_of(c * wide, wide), wide)
            taken = rows_ref[g].reshape(rows, model)
            gate = jnp.dot(taken, gate_ref[:, cut], preferred_element_type=jnp.float32)
            upward = jnp.dot(taken, up_ref[:, cut], preferred_element_type=jnp.float32)
            hidden_ref[:, cut] = (gate / (1.0 + jnp.exp(-gate)) * upward).astype(hidden_ref.dtype)

        @pl.loop(0, model // wide)
        def _(c):
            cut = pl.ds(pl.multiple_of(c * wide, wide), wide)
            product = jnp.dot(
                hidden_ref[...], down_ref[:, cut], preferred_element_type=jnp.float32
            ).astype(part_ref.dtype)
            part_ref[g, :, :, :, cut] = product.reshape(part_ref.shape[1:4] + (wide,))

        swap(g).start()
        swap(g).wait_recv()
        for j in range(per):
            mine = part_ref[g, core, j].astype(jnp.float32)
            sum_ref[g, j] = (mine + far_ref[g, j].astype(jnp.float32)).astype(sum_ref.dtype)
            if j > 0:

                @pl.when(g + j > 1)
                def _():
                    home(g, j - 1).start()

        home(g, per - 1).start()

    back_ref[me] = sum_ref[0, 0]

    @pl.loop(1, count)
    def _(step):
        g, j = step // per, step % per
        came_home(g, j).wait_recv()
        home(g, j).wait_send()
        across(g, j).wait_send()

    @pl.loop(0, count)
    def _(step):
        forward(step // per, step % per, core).wait_send()

    @pl.loop(0, groups)
    def _(g):
        swap(g).wait_send()


def run_experts(count, outgoing, gate_weight, up_weight, down_weight):
    _, capacity, model = outgoing.shape
    per = REACH + 1
    groups = count // per
    hidden = gate_weight.shape[1]
    kept = outgoing.dtype
    each = pltpu.SemaphoreType.DMA((groups, per))
    whole = pltpu.SemaphoreType.DMA((groups,))
    anywhere = pl.BlockSpec(memory_space=pl.ANY)
    return pl.pallas_call(
        functools.partial(experts_kernel, count),
        out_shape=jax.ShapeDtypeStruct(outgoing.shape, kept),
        in_specs=[VMEM, anywhere, anywhere, anywhere],
        out_specs=VMEM,
        scratch_shapes=[
            pltpu.VMEM((groups, 2, per, capacity, model), kept),
            pltpu.VMEM((groups, 2, per, capacity, model), kept),
            pltpu.VMEM((groups, per, capacity, model), kept),
            pltpu.VMEM((groups, per, capacity, model), kept),
            pltpu.VMEM((2 * per * capacity, hidden), kept),
            pltpu.VMEM(gate_weight.shape, kept),
            pltpu.VMEM(up_weight.shape, kept),
            pltpu.VMEM(down_weight.shape, kept),
            pltpu.SemaphoreType.DMA((3,)),
            pltpu.SemaphoreType.DMA,
            each,
            each,
            each,
            each,
            whole,
            whole,
            each,
            each,
        ],
        compiler_params=pltpu.CompilerParams(collective_id=1, has_side_effects=True),
        name="experts",
    )(outgoing, gate_weight, up_weight, down_weight)


def slots_of(routes, experts, capacity):
    flat_routes = routes.reshape(-1)
    table = (flat_routes[:, None] == jnp.arange(experts, dtype=jnp.int32)[None, :]).astype(
        jnp.float32
    )
    count = table.shape[0]
    before = jnp.tril(jnp.ones((count, count), jnp.bfloat16), -1)
    earlier = jnp.dot(before, table.astype(jnp.bfloat16), preferred_element_type=jnp.float32)
    rank = jnp.sum(earlier * table, axis=1).astype(jnp.int32)
    return (flat_routes * capacity + rank).reshape(routes.shape)


def on_device(
    residual,
    query_rows,
    key_rows,
    value_rows,
    mix_lambda,
    documents,
    out_weight,
    norm_gain,
    gate_weight,
    up_weight,
    down_weight,
    routes,
    route_weights,
):
    length = query_rows.shape[0]
    model_width = residual.shape[1]
    experts = lax.axis_size("sp")
    capacity = 2 * length // experts
    top_count = routes.shape[1]
    keys, values, ids = halo(experts, key_rows, value_rows, documents.reshape(1, length))
    merged = attention(
        query_rows,
        keys.reshape(-1, keys.shape[-1]),
        values.reshape(-1, values.shape[-1]),
        documents.reshape(length, 1),
        ids.reshape(1, -1),
        mix_lambda,
    )
    token_heads = lax.all_to_all(merged, "tp", split_axis=0, concat_axis=1, tiled=True)
    projected = jnp.dot(token_heads, out_weight, preferred_element_type=jnp.float32)
    mixed = (residual.astype(jnp.float32) + projected).astype(jnp.bfloat16)
    mixed_wide = mixed.astype(jnp.float32)
    normed = (
        mixed_wide
        * lax.rsqrt(jnp.mean(mixed_wide * mixed_wide, axis=-1, keepdims=True) + 1e-06)
        * norm_gain
    ).astype(jnp.bfloat16)
    slots = slots_of(routes, experts, capacity)
    places = jnp.arange(experts * capacity, dtype=jnp.int32)
    spread = jnp.any(slots[None, :, :] == places[:, None, None], axis=-1).astype(jnp.bfloat16)
    outgoing = jnp.dot(spread, normed, preferred_element_type=jnp.float32).astype(jnp.bfloat16)
    returned = run_experts(
        experts,
        outgoing.reshape(experts, capacity, model_width),
        gate_weight[0],
        up_weight[0],
        down_weight[0],
    ).reshape(-1, model_width)
    weighted = 0.0
    for which in range(top_count):
        pick = (slots[:, which][:, None] == places[None, :]).astype(jnp.bfloat16)
        picked = jnp.dot(pick, returned, preferred_element_type=jnp.float32)
        weighted = weighted + picked * route_weights[:, which][:, None]
    return (mixed_wide + weighted).astype(jnp.bfloat16)


def solution(mesh):
    placed = (
        P(("sp", "tp"), None),
        P("sp", "tp"),
        P("sp", "tp"),
        P("sp", "tp"),
        P("tp"),
        P("sp"),
        P(),
        P(),
        P("sp", None, "tp"),
        P("sp", None, "tp"),
        P("sp", "tp", None),
        P(("sp", "tp"), None),
        P(("sp", "tp"), None),
    )
    return jax.shard_map(
        on_device, mesh=mesh, in_specs=placed, out_specs=P(("sp", "tp"), None), check_vma=False
    )
```
